32 devices in a mesh: grp: 2 (over y), ep: 4 (over z), tp: 4 (over x, core).
Axes of the slice: x: 2, y: 2, z: 4, core: 2. Of those that a mesh axis runs over, the one named last changes fastest.
Arguments:
- queries: bfloat16 [1024, 16, 128], P(('grp', 'ep'), 'tp'), parts along dimension 0, may hold values from -6 to 6
- key_vectors: bfloat16 [1024, 16, 128], P(('grp', 'ep'), 'tp'), parts along dimension 0, may hold values from -6 to 6
- values: bfloat16 [1024, 16, 128], P(('grp', 'ep'), 'tp'), parts along dimension 0, may hold values from -6 to 6
- forget_cum: float32 [1024, 16], P('grp', 'tp'), parts along dimension 0, may hold values from -90 to 0, as said below
- query_gain: float32 [128], replicated, may hold values from 0.1 to 5.5
- key_gain: float32 [128], replicated, may hold values from 0.1 to 5.5
- tokens: bfloat16 [4096, 4096], P(('grp', 'ep', 'tp')), parts along dimension 0, may hold values from -6 to 6
- norm_gain: float32 [4096], replicated, may hold values from 0.1 to 1.9
- routes: int32 [4096, 2], P(('grp', 'ep', 'tp')), parts along dimension 0, may hold values from 0 to 127, all different within a row; in each aligned block of 128 rows (0 to 127, 128 to 255, ...) at most 2 rows name the same one
- route_weights: float32 [4096, 2], P(('grp', 'ep', 'tp')), parts along dimension 0, may hold values from 0.3 to 1.2
- expert_gate: bfloat16 [128, 4096, 384], P(('ep', 'tp')), may hold values from -0.09375 to 0.09375
- expert_up: bfloat16 [128, 4096, 384], P(('ep', 'tp')), may hold values from -0.09375 to 0.09375
- expert_down: bfloat16 [128, 384, 4096], P(('ep', 'tp')), may hold values from -0.3125 to 0.3125
- shared_gate: bfloat16 [4096, 192], P(None, 'tp'), may hold values from -0.09375 to 0.09375
- shared_up: bfloat16 [4096, 192], P(None, 'tp'), may hold values from -0.09375 to 0.09375
- shared_down: bfloat16 [192, 4096], P('tp'), may hold values from -0.4375 to 0.4375
Outputs:
- attended: bfloat16 [1024, 16, 128], P(('grp', 'ep'), 'tp'), parts along dimension 0
- routed_output: bfloat16 [4096, 4096], P(('grp', 'ep', 'tp')), parts along dimension 0
The draws below stay inside these ranges and needn't reach their ends.
There are 2 independent parts, one for each index of `grp`. The reference program is written for one: setup_inputs(seed, part) draws one part's arguments, and reference() takes and returns one part's arrays. A program takes and returns all parts, laid end to end along the dimension named above; an argument that names none is the same for every part. Nothing has to cross between parts.
Inputs may be any that keep to these rules, and one draw needn't show every extreme that they name: `routes`: each row names 2 different experts; the rows of one device name every expert exactly 2 times. `forget_cum`: never rises from one position to the next.
All inputs are finite; a program needn't handle non-finite values.
Results may differ from the reference program's by a relative error of at most 0.007.
The reference program's roundings to bfloat16 on the way count: a program that leaves them out, or rounds other values in their place, can miss the bound.
Values may be sent and summed in bfloat16 or wider, within the bound.
A program may use at most 128 MiB of HBM per device.

```python
import math
import jax
import jax.numpy as jnp
import numpy as np
from jax import lax

D = 4096
HEADS = 16
HD = 128
EXPERTS = 128
EF = 384
SF = 192
TOP_K = 2
TOKENS_PER_SHARD = 128
TOK_B = 128
CAP = 2
SEQUENCE_LENGTH = 512
TOKENS_B = 2048
N_EP = 4
N_TP = 4


def query_key_pair(key):
    query_base = jnp.clip(jax.random.normal(jax.random.fold_in(key, 701), (SEQUENCE_LENGTH, HEADS, HD), jnp.float32), -6.0, 6.0)
    key_base = jnp.clip(jax.random.normal(jax.random.fold_in(key, 702), (SEQUENCE_LENGTH, HEADS, HD), jnp.float32), -6.0, 6.0)
    return (query_base, key_base)


def draw_queries(key, part):
    return query_key_pair(key)[0].astype(jnp.bfloat16)


def draw_key_vectors(key, part):
    return query_key_pair(key)[1].astype(jnp.bfloat16)


def gain_sample(key):
    return 1.0 + jnp.clip(0.18 * jax.random.normal(key, (HD,), jnp.float32), -0.9, 0.9)


def draw_query_gain(key, part):
    return gain_sample(jax.random.fold_in(key, 801))


def draw_key_gain(key, part):
    return gain_sample(jax.random.fold_in(key, 802))


def draw_forget_cum(key, part):
    order = jax.random.permutation(jax.random.fold_in(key, 901), HEADS)
    gentle_decay = (order < HEADS // 2).astype(jnp.float32)
    totals = jnp.exp(jax.random.uniform(jax.random.fold_in(key, 902), (HEADS,), jnp.float32, jnp.log(0.3), jnp.log(1.0))) / SEQUENCE_LENGTH
    quick = jnp.exp(jax.random.uniform(jax.random.fold_in(key, 903), (HEADS,), jnp.float32, jnp.log(1.0 / 60.0), jnp.log(1.0 / 25.0)))
    decay_speed = gentle_decay * totals + (1.0 - gentle_decay) * quick
    block_multiplier = jnp.exp(jax.random.uniform(jax.random.fold_in(key, 904), (SEQUENCE_LENGTH // TOKENS_PER_SHARD,), jnp.float32, jnp.log(0.35), jnp.log(2.8)))
    jagged_profile = jax.random.uniform(jax.random.fold_in(key, 905), (SEQUENCE_LENGTH, HEADS), jnp.float32, 0.5, 1.5)
    position_indices = jnp.arange(SEQUENCE_LENGTH)
    spike_position = jax.random.randint(jax.random.fold_in(key, 906), (3,), 0, SEQUENCE_LENGTH)
    spike_magnitude = jax.random.uniform(jax.random.fold_in(key, 907), (3,), jnp.float32, 0.22, 0.69)
    forget_spike = jnp.sum(jnp.where(position_indices[:, None] == spike_position[None, :], spike_magnitude[None, :], 0.0), axis=1)
    forget_logarithm = -(decay_speed[None, :] * jnp.repeat(block_multiplier, TOKENS_PER_SHARD)[:, None] * jagged_profile) - forget_spike[:, None] * gentle_decay[None, :]
    return jnp.cumsum(forget_logarithm, axis=0)


def block_levels(stream_key, shape, shards, least, top_value):
    gain, own = 1.0, jax.random.fold_in(stream_key, 6)
    for dim, parts in shards:
        draws = jnp.exp(jax.random.uniform(jax.random.fold_in(own, dim), (parts,), jnp.float32, least / len(shards), top_value / len(shards)))
        gain = gain * jnp.repeat(draws, shape[dim] // parts).reshape([-1 if axis == dim else 1 for axis in range(len(shape))])
    return gain


def deal_out(own_key, own, number, rows, amount, top, most, lean):
    order = jax.random.permutation(own_key, amount)
    heavy_load, usual = portions_of(amount, rows * top, most, lean, True), portions_of(amount, rows * top, most, lean, False)
    places = jnp.arange(amount)

    def named(sizes, rotation):
        used = int((sizes > 0).sum())
        fixed = max(1, used // 4)
        passed = fixed + (places - fixed + rotation * (used - fixed)) % max(1, amount - fixed)
        return jnp.zeros((amount,), jnp.int32).at[order[jnp.where(places < fixed, places, passed)]].set(jnp.asarray(sizes, jnp.int32))

    sizes = jnp.where(number % 4 == 0, named(heavy_load, number // 4), named(usual, number - number // 4 - 1))
    mixed = jax.random.permutation(jax.random.fold_in(own, 3), amount)
    source_of, taker = mixed[0:amount // 2 * 2:2], mixed[1:amount // 2 * 2:2]
    margin = jnp.minimum(sizes[source_of] - 1, most - sizes[taker]) // 2
    margin = jnp.where((source_of == order[0]) | (taker == order[0]) | (sizes[taker] == 0), 0, jnp.maximum(margin, 0))
    passed = jax.random.randint(jax.random.fold_in(own, 4), (amount // 2,), 0, 1 << 20) % (margin + 1)
    sizes = sizes.at[source_of].add(-passed).at[taker].add(passed)
    items = jnp.searchsorted(jnp.cumsum(sizes), jnp.arange(rows * top), side="right").astype(jnp.int32)
    grid = items.reshape(top, rows).T
    grid = grid[jax.random.permutation(jax.random.fold_in(own, 1), rows)]
    rotation = jax.random.randint(jax.random.fold_in(own, 2), (rows, 1), 0, top)
    return jnp.take_along_axis(grid, (jnp.arange(top)[None, :] + rotation) % top, axis=1)


def portions_of(number_of, total, limit, skew, full):
    loads = [(1 << 20) // math.isqrt(grade ** skew) + 1 for grade in range(1, number_of + 1)]
    largest = limit if full else min(limit, max(-(-total // number_of), total * loads[0] // sum(loads)))
    least = 1 if total - largest >= number_of - 1 else 0
    counts, surplus = [largest] + [least] * (number_of - 1), total - largest - least * (number_of - 1)
    while surplus > 0:
        movable = [i for i in range(1, number_of) if counts[i] < largest] or [i for i in range(1, number_of) if counts[i] < limit]
        mass, budget = sum([loads[i] for i in movable]), surplus
        for i in movable:
            addition = min(limit - counts[i], max(1, budget * loads[i] // mass), surplus)
            counts[i] = counts[i] + addition
            surplus = surplus - addition
    return np.array(counts)


def scatter_about(key, dims, width, most, shards=(), held_as=jnp.bfloat16):
    level = block_levels(key, dims, shards, -0.22, 0.18) if shards else 1.0
    drawn = jax.random.normal(key, dims, jnp.float32) * width * level
    return jnp.minimum(jnp.maximum(drawn, -most), most).astype(held_as)


def setup_inputs(seed: int = 0, part: int = 0) -> dict:
    streams_of = jax.random.split(jax.random.key(seed), 17)
    part_keys = jax.random.split(jax.random.fold_in(streams_of[16], part), 17)
    queries = draw_queries(jax.random.fold_in(jax.random.fold_in(streams_of[16], part), 71), part)
    key_vectors = draw_key_vectors(jax.random.fold_in(jax.random.fold_in(streams_of[16], part), 71), part)
    values = scatter_about(part_keys[2], (SEQUENCE_LENGTH, HEADS, HD), 1.0, 6.0, ((0, 4), (1, 4)))
    forget_cum = draw_forget_cum(jax.random.fold_in(jax.random.fold_in(streams_of[16], part), 71), part)
    query_gain = draw_query_gain(jax.random.fold_in(streams_of[16], 71), part)
    key_gain = draw_key_gain(jax.random.fold_in(streams_of[16], 71), part)
    tokens = scatter_about(part_keys[6], (TOKENS_B, D), 1.0, 6.0, ((0, 16),))
    norm_gain = jnp.clip(1.0 + 0.18 * jax.random.normal(streams_of[7], (D,), jnp.float32), 0.1, 1.9)
    routes_keys = jax.random.split(jax.random.fold_in(part_keys[8], 1), TOKENS_B // TOK_B)
    routes_turns = jax.random.permutation(jax.random.fold_in(part_keys[8], 3), TOKENS_B // TOK_B)
    routes = jax.vmap(lambda own, number: deal_out(jax.random.fold_in(part_keys[8], 2), own, number, TOK_B, EXPERTS, TOP_K, CAP, 0))(routes_keys, routes_turns).reshape((TOKENS_B, TOP_K))
    route_weights = jnp.clip(0.3 + 0.90000004 * jax.random.uniform(part_keys[9], (TOKENS_B, TOP_K), jnp.float32) ** block_levels(part_keys[9], (TOKENS_B, TOP_K), ((0, 16),), -0.2, 0.2), 0.3, 1.2)
    expert_gate = scatter_about(streams_of[10], (EXPERTS, D, EF), D ** -0.5, 0.09375, ((0, 16),))
    expert_up = scatter_about(streams_of[11], (EXPERTS, D, EF), D ** -0.5, 0.09375, ((0, 16),))
    expert_down = scatter_about(streams_of[12], (EXPERTS, EF, D), EF ** -0.5, 0.3125, ((0, 16),))
    shared_gate = scatter_about(streams_of[13], (D, SF), D ** -0.5, 0.09375, ((1, 4),))
    shared_up = scatter_about(streams_of[14], (D, SF), D ** -0.5, 0.09375, ((1, 4),))
    shared_down = scatter_about(streams_of[15], (SF, D), SF ** -0.5, 0.4375, ((0, 4),))
    return {"queries": queries, "key_vectors": key_vectors, "values": values, "forget_cum": forget_cum, "query_gain": query_gain, "key_gain": key_gain, "tokens": tokens, "norm_gain": norm_gain, "routes": routes, "route_weights": route_weights, "expert_gate": expert_gate, "expert_up": expert_up, "expert_down": expert_down, "shared_gate": shared_gate, "shared_up": shared_up, "shared_down": shared_down}


def rms_rows(row_values, gain_vector):
    widened = row_values.astype(jnp.float32)
    inverse = lax.rsqrt(lax.optimization_barrier(jnp.mean(widened * widened, axis=-1, keepdims=True)) + 1e-06)
    return (widened * inverse * gain_vector.astype(jnp.float32)).astype(jnp.bfloat16)

def attention(queries, key_vectors, values, forget_cum, query_gain, key_gain):
    query_norm = lax.optimization_barrier(rms_rows(queries, query_gain)).astype(jnp.float32)
    key_norm = lax.optimization_barrier(rms_rows(key_vectors, key_gain)).astype(jnp.float32)
    value_wide = values.astype(jnp.float32)
    length = queries.shape[0]
    block_rows = 512 if length % 512 == 0 else length
    scale_factor = queries.shape[2] ** (-0.5)
    outputs = []
    for first_row in range(0, length, block_rows):
        stop_row = first_row + block_rows
        scores = jnp.einsum('qhd,khd->hqk', query_norm[first_row:stop_row], key_norm[:stop_row]) * scale_factor
        scores = scores + forget_cum[first_row:stop_row].T[:, :, None] - forget_cum[:stop_row].T[:, None, :]
        allowed = (jnp.arange(stop_row)[None, :] <= jnp.arange(first_row, stop_row)[:, None])[None]
        scores = jnp.where(allowed, scores, -jnp.inf)
        row_max = lax.optimization_barrier(jnp.max(scores, axis=2, keepdims=True))
        weights = jnp.exp(scores - row_max)
        denominator = lax.optimization_barrier(jnp.sum(weights, axis=2))
        probabilities = lax.optimization_barrier(weights.astype(jnp.bfloat16)).astype(jnp.float32)
        mixed_rows = jnp.einsum('hqk,khd->hqd', probabilities, value_wide[:stop_row]) / denominator[:, :, None]
        outputs.append(mixed_rows.transpose(1, 0, 2))
    return jnp.concatenate(outputs, axis=0).astype(jnp.bfloat16)

def mixture(tokens, norm_gain, routes, route_weights, expert_gate, expert_up, expert_down, shared_gate, shared_up, shared_down):
    normed = rms_rows(tokens, norm_gain)
    row_total = tokens.shape[0]
    shared_hidden = (jax.nn.silu(jnp.dot(normed, shared_gate, preferred_element_type=jnp.float32)) * jnp.dot(normed, shared_up, preferred_element_type=jnp.float32)).astype(jnp.bfloat16)
    part_width = shared_down.shape[0] // N_TP
    shared_sum = jnp.zeros((row_total, tokens.shape[1]), jnp.float32)
    for block_index in range(N_TP):
        low = block_index * part_width
        partial_value = jnp.dot(shared_hidden[:, low:low + part_width], shared_down[low:low + part_width], preferred_element_type=jnp.float32)
        shared_sum = shared_sum + lax.optimization_barrier(partial_value.astype(jnp.bfloat16)).astype(jnp.float32)
    shared_out = shared_sum.astype(jnp.bfloat16)
    block_count = N_EP * N_TP
    per_block = routes.reshape(block_count, -1)
    choices_per = per_block.shape[1]
    token_index = (jnp.arange(block_count)[:, None] * (choices_per // TOP_K) + jnp.arange(choices_per)[None, :] // TOP_K).astype(jnp.int32)
    weight_table = route_weights.reshape(block_count, -1)
    one_hot = (per_block[:, :, None] == jnp.arange(EXPERTS)[None, None, :]).astype(jnp.int32)
    slot_rank = lax.optimization_barrier(jnp.sum((jnp.cumsum(one_hot, axis=1) - one_hot) * one_hot, axis=2))

    def one_expert(running_sum, expert_index):
        chosen = per_block == expert_index
        placed = chosen[:, :, None] & (slot_rank[:, :, None] == jnp.arange(CAP)[None, None, :])
        row_ids = lax.optimization_barrier(jnp.sum(jnp.where(placed, token_index[:, :, None], 0), axis=1)).reshape(-1).astype(jnp.int32)
        slot_weight = lax.optimization_barrier(jnp.sum(jnp.where(placed, weight_table[:, :, None], 0.0), axis=1)).reshape(-1)
        picked = normed[row_ids]
        gate_values = jnp.dot(picked, expert_gate[expert_index], preferred_element_type=jnp.float32)
        upward = jnp.dot(picked, expert_up[expert_index], preferred_element_type=jnp.float32)
        hidden = (jax.nn.silu(gate_values) * upward).astype(jnp.bfloat16)
        produced = jnp.dot(hidden, expert_down[expert_index], preferred_element_type=jnp.float32).astype(jnp.bfloat16)
        produced = lax.optimization_barrier(produced).astype(jnp.float32)
        return (running_sum.at[row_ids].add(slot_weight[:, None] * produced), None)
    routed, _ = lax.scan(one_expert, jnp.zeros((row_total, tokens.shape[1]), jnp.float32), jnp.arange(EXPERTS).astype(jnp.int32))
    return (shared_out.astype(jnp.float32) + routed).astype(jnp.bfloat16)

def reference(queries, key_vectors, values, forget_cum, query_gain, key_gain, tokens, norm_gain, routes, route_weights, expert_gate, expert_up, expert_down, shared_gate, shared_up, shared_down):
    attended = attention(queries, key_vectors, values, forget_cum, query_gain, key_gain)
    routed_output = mixture(tokens, norm_gain, routes, route_weights, expert_gate, expert_up, expert_down, shared_gate, shared_up, shared_down)
    return (attended, routed_output)
```

```python
import functools
import jax
import jax.numpy as jnp
from jax import lax
from jax.experimental import pallas as pl
from jax.experimental.pallas import tpu as pltpu
from jax.sharding import PartitionSpec as P

MESH = pl.DeviceIdType.MESH
F32 = jnp.float32
BF16 = jnp.bfloat16
CAP = 2
CHUNKS = 4
SLOTS = 4

D = 4096
EXPERTS = 128
TOP_K = 2


def rms_rows(row_values, gain_vector):
    widened = row_values.astype(jnp.float32)
    inverse = lax.rsqrt(jnp.mean(widened * widened, axis=-1, keepdims=True) + 1e-06)
    return (widened * inverse * gain_vector).astype(jnp.bfloat16)


def attend(queries, key_vectors, values, forget_cum, query_gain, key_gain):
    query_norm = rms_rows(queries, query_gain)
    key_norm = rms_rows(key_vectors, key_gain)
    query_rows = query_norm.shape[0]
    head_count = query_norm.shape[1]
    head_size = query_norm.shape[2]
    first_query = lax.axis_index("ep") * query_rows
    query_positions = first_query + lax.iota(jnp.int32, query_rows)
    last_query = first_query + query_rows - 1
    query_cum = lax.dynamic_slice_in_dim(forget_cum, first_query, query_rows, 0).T
    scale_factor = head_size ** (-0.5)
    start_state = (
        jnp.full((head_count, query_rows), -1e30, jnp.float32),
        jnp.zeros((head_count, query_rows), jnp.float32),
        jnp.zeros((head_count, query_rows, head_size), jnp.float32),
    )
    key_part = lax.all_gather(key_norm, "ep", axis=0, tiled=True)
    value_part = lax.all_gather(values, "ep", axis=0, tiled=True)
    piece_rows = key_part.shape[0]

    def compute(inner_state):
        best_score, denominator, accumulated = inner_state
        cum_block = forget_cum.T
        scores = jnp.einsum(
            "qhd,khd->hqk", query_norm, key_part, preferred_element_type=jnp.float32
        )
        scores = scores * scale_factor + query_cum[:, :, None] - cum_block[:, None, :]
        key_positions = lax.iota(jnp.int32, piece_rows)
        allowed = (key_positions[None, :] <= query_positions[:, None])[None]
        scores = jnp.where(allowed, scores, -1e30)
        new_best = jnp.maximum(best_score, jnp.max(scores, axis=2))
        weights = jnp.where(allowed, jnp.exp(scores - new_best[:, :, None]), 0.0)
        denominator = jnp.sum(weights, axis=2)
        product = jnp.einsum(
            "hqk,khd->hqd",
            weights.astype(jnp.bfloat16),
            value_part,
            preferred_element_type=jnp.float32,
        )
        accumulated = product
        return (new_best, denominator, accumulated)

    best_score, denominator, accumulated = lax.cond(
        jnp.int32(0) <= last_query, compute, lambda inner_state: inner_state, start_state
    )
    return (accumulated / denominator[:, :, None]).transpose(1, 0, 2).astype(jnp.bfloat16)


def shared_expert(normed, shared_gate, shared_up, shared_down):
    row_count = normed.shape[0]
    whole_gate, whole_up, whole_down = (
        lax.all_gather(shared_gate, "tp", axis=1, tiled=True),
        lax.all_gather(shared_up, "tp", axis=1, tiled=True),
        lax.all_gather(shared_down, "tp", axis=0, tiled=True),
    )
    block_total = lax.axis_size("tp")
    gate_values = jnp.dot(normed, whole_gate, preferred_element_type=jnp.float32)
    upward = jnp.dot(normed, whole_up, preferred_element_type=jnp.float32)
    hidden_whole = (jax.nn.silu(gate_values) * upward).astype(jnp.bfloat16)
    part_width = whole_down.shape[0] // block_total
    hidden_blocks = hidden_whole.reshape(row_count, block_total, part_width)
    down_blocks = whole_down.reshape(block_total, part_width, whole_down.shape[1])
    partials = jnp.einsum(
        "rnp,npd->nrd", hidden_blocks, down_blocks, preferred_element_type=jnp.float32
    ).astype(jnp.bfloat16)
    return jnp.sum(partials.astype(jnp.float32), axis=0).astype(jnp.bfloat16)


def mixture(
    tokens,
    norm_gain,
    routes,
    route_weights,
    expert_gate,
    expert_up,
    expert_down,
    shared_gate,
    shared_up,
    shared_down,
):
    normed = rms_rows(tokens, norm_gain)
    row_count = tokens.shape[0]
    shared_out = shared_expert(normed, shared_gate, shared_up, shared_down)
    flat_routes = routes.reshape(-1)
    choice_count = flat_routes.shape[0]
    one_hot = (flat_routes[:, None] == lax.iota(jnp.int32, EXPERTS)[None, :]).astype(jnp.int32)
    slot_rank = jnp.sum((jnp.cumsum(one_hot, axis=0) - one_hot) * one_hot, axis=1)
    slot_index = slot_rank * EXPERTS + flat_routes
    slot_ids = lax.iota(jnp.int32, CAP * EXPERTS)
    matches = slot_index[None, :] == slot_ids[:, None]
    source_row = jnp.sum(
        jnp.where(matches, lax.iota(jnp.int32, choice_count)[None, :] // TOP_K, 0), axis=1
    )
    filled = jnp.any(matches, axis=1)
    outgoing = jnp.where(filled[:, None], normed[source_row], jnp.zeros((), jnp.bfloat16)).reshape(
        CAP, EXPERTS, D
    )
    arrived = lax.all_to_all(outgoing, ("ep", "tp"), split_axis=1, concat_axis=1, tiled=True)
    local_count = expert_gate.shape[0]
    grouped = arrived.reshape(CAP, -1, local_count, D)
    gate_values = jnp.einsum(
        "csed,edf->csef", grouped, expert_gate, preferred_element_type=jnp.float32
    )
    upward = jnp.einsum("csed,edf->csef", grouped, expert_up, preferred_element_type=jnp.float32)
    hidden = (jax.nn.silu(gate_values) * upward).astype(jnp.bfloat16)
    produced = (
        jnp.einsum("csef,efd->csed", hidden, expert_down, preferred_element_type=jnp.float32)
        .astype(jnp.bfloat16)
        .reshape(CAP, -1, D)
    )
    returned = lax.all_to_all(produced, ("ep", "tp"), split_axis=1, concat_axis=1, tiled=True)
    picked_rows = returned.reshape(CAP * EXPERTS, D)[slot_index].reshape(row_count, TOP_K, D)
    routed = jnp.sum(route_weights[:, :, None] * picked_rows.astype(jnp.float32), axis=1)
    return (shared_out.astype(jnp.float32) + routed).astype(jnp.bfloat16)


def local(
    queries,
    key_vectors,
    values,
    forget_cum,
    query_gain,
    key_gain,
    tokens,
    norm_gain,
    routes,
    route_weights,
    expert_gate,
    expert_up,
    expert_down,
    shared_gate,
    shared_up,
    shared_down,
):
    attended = attend(queries, key_vectors, values, forget_cum, query_gain, key_gain)
    routed_output = mixture(
        tokens,
        norm_gain,
        routes,
        route_weights,
        expert_gate,
        expert_up,
        expert_down,
        shared_gate,
        shared_up,
        shared_down,
    )
    return (attended, routed_output)


def rms_heads(wide, gain, heads, size):
    pieces = []
    for h in range(heads):
        part = wide[:, h * size : (h + 1) * size]
        inverse = lax.rsqrt(jnp.mean(part * part, axis=-1, keepdims=True) + 1e-06)
        pieces.append((part * inverse * gain).astype(BF16))
    return jnp.concatenate(pieces, axis=1)


def prepare_kernel(
    local_count,
    heads,
    tokens_ref,
    gain_ref,
    routes_ref,
    routes_t_ref,
    weights_ref,
    q_ref,
    k_ref,
    qg_ref,
    kg_ref,
    normed_ref,
    out_ref,
    high_ref,
    low_ref,
    qn_ref,
    kn_ref,
):
    size = qg_ref.shape[1]
    qn_ref[...] = rms_heads(q_ref[...].astype(F32), qg_ref[...], heads, size)
    kn_ref[...] = rms_heads(k_ref[...].astype(F32), kg_ref[...], heads, size)
    rows = tokens_ref.shape[0]
    slots = out_ref.shape[0]
    group = CAP * local_count

    def expert_of(r):
        return (r // group) * local_count + r % local_count

    def rank_of(r):
        return ((r % group) // local_count).astype(F32)

    r = lax.broadcasted_iota(jnp.int32, (slots, rows), 0)
    expert = expert_of(r)
    named = (expert == routes_t_ref[0:1, :]) | (expert == routes_t_ref[1:2, :])
    named = jnp.where(named, 1.0, 0.0)
    a = lax.broadcasted_iota(jnp.int32, (rows, rows), 0)
    b = lax.broadcasted_iota(jnp.int32, (rows, rows), 1)
    before = jnp.where(a < b, 1.0, 0.0).astype(BF16)
    earlier = jnp.dot(named.astype(BF16), before, preferred_element_type=F32)
    pick = jnp.where(earlier == rank_of(r), named, 0.0).astype(BF16)
    r = lax.broadcasted_iota(jnp.int32, (rows, slots), 1)
    expert = expert_of(r)
    first = expert == routes_ref[:, 0:1]
    second = expert == routes_ref[:, 1:2]
    named = jnp.where(first | second, 1.0, 0.0)
    after = jnp.where(b < a, 1.0, 0.0).astype(BF16)
    earlier = jnp.dot(after, named.astype(BF16), preferred_element_type=F32)
    weight = jnp.where(first, weights_ref[:, 0:1], weights_ref[:, 1:2])
    weight = jnp.where(earlier == rank_of(r), named * weight, 0.0)
    high = weight.astype(BF16)
    high_ref[...] = high
    low_ref[...] = (weight - high.astype(F32)).astype(BF16)

    wide = tokens_ref[...].astype(F32)
    inverse = lax.rsqrt(jnp.mean(wide * wide, axis=-1, keepdims=True) + 1e-06)
    width = tokens_ref.shape[1] // 8
    for c in range(8):
        cols = slice(c * width, (c + 1) * width)
        piece = (tokens_ref[:, cols].astype(F32) * inverse * gain_ref[:, cols]).astype(BF16)
        normed_ref[:, cols] = piece
        out_ref[:, cols] = jnp.dot(pick, piece, preferred_element_type=F32).astype(BF16)


def fused_kernel(
    n_ep,
    n_tp,
    heads,
    normed_ref,
    high_ref,
    low_ref,
    qn_ref,
    qc_ref,
    kc_ref,
    outgoing_ref,
    kn_ref,
    v_ref,
    gate_ref,
    up_ref,
    down_ref,
    shared_ref,
    att_ref,
    res_ref,
    x_buf,
    y_buf,
    r_buf,
    ring,
    down_buf,
    sh_buf,
    kv_buf,
    acc_g,
    acc_u,
    hid,
    sh_out,
    x_send,
    x_recv,
    x_own,
    y_send,
    y_recv,
    y_own,
    ring_sem,
    down_sem,
    sh_send,
    sh_recv,
    sh_own,
    sf_send,
    sf_recv,
    kv_send,
    kv_recv,
    kv_own,
):
    e_pos = lax.axis_index("ep")
    t_pos = lax.axis_index("tp")
    count = n_ep * n_tp
    me = e_pos * n_tp + t_pos
    local_count = gate_ref.shape[0]
    group = CAP * local_count
    slots = count * group
    wide = x_buf.shape[2]
    steps = CHUNKS * local_count
    peer_rows = (count - 1) * group

    def device(i):
        return {"ep": i // n_tp, "tp": i % n_tp}

    def weight_copies(n, slot):
        rows = pl.ds(pl.multiple_of((n // local_count) * wide, wide), wide)
        e = n % local_count
        return (
            pltpu.make_async_copy(gate_ref.at[e, rows], ring.at[slot, 0], ring_sem.at[slot, 0]),
            pltpu.make_async_copy(up_ref.at[e, rows], ring.at[slot, 1], ring_sem.at[slot, 1]),
        )

    barrier = pltpu.get_barrier_semaphore()

    def greet(i, carry):
        pl.semaphore_signal(
            barrier, inc=1, device_id=device((me + i) % count), device_id_type=MESH
        )
        return carry

    lax.fori_loop(1, count, greet, 0)
    for n in range(SLOTS):
        for copy in weight_copies(n, n):
            copy.start()
    down_copy = pltpu.make_async_copy(down_ref, down_buf, down_sem)
    down_copy.start()
    own_kv = [
        pltpu.make_async_copy(src, kv_buf.at[e_pos, j], kv_own.at[j])
        for j, src in enumerate((kn_ref, v_ref))
    ]
    for copy in own_kv:
        copy.start()
    own_shared = pltpu.make_async_copy(shared_ref, sh_buf.at[t_pos], sh_own)
    own_shared.start()
    for blk in range(n_ep):

        @pl.when(blk > e_pos)
        def _():
            kv_buf[blk] = jnp.zeros(kv_buf.shape[1:], BF16)

    pl.semaphore_wait(barrier, count - 1)

    def rows_of(i):
        return pl.ds(pl.multiple_of(i * group, group), group)

    def dispatch(c):
        cols = pl.ds(c * wide, wide)
        pltpu.make_async_copy(
            outgoing_ref.at[rows_of(me), cols], x_buf.at[c, rows_of(me)], x_own.at[c]
        ).start()

        def send(i, carry):
            peer = (me + i) % count
            pltpu.make_async_remote_copy(
                src_ref=outgoing_ref.at[rows_of(peer), cols],
                dst_ref=x_buf.at[c, rows_of(me)],
                send_sem=x_send.at[c],
                recv_sem=x_recv.at[c],
                device_id=device(peer),
                device_id_type=MESH,
            ).start()
            return carry

        lax.fori_loop(1, count, send, 0)

    def kv_copy(step, src_k, src_v):
        blk = jnp.maximum(e_pos - step, 0)
        nxt = jnp.minimum(e_pos + 1, n_ep - 1)
        return [
            pltpu.make_async_remote_copy(
                src_ref=src,
                dst_ref=kv_buf.at[blk, j],
                send_sem=kv_send.at[step, j],
                recv_sem=kv_recv.at[step, j],
                device_id={"ep": nxt},
                device_id_type=MESH,
            )
            for j, src in enumerate((src_k, src_v))
        ]

    def kv_arrived(step):
        blk = jnp.maximum(e_pos - 1 - step, 0)

        @pl.when(e_pos - 1 - step >= 0)
        def _():
            for j in range(2):
                pltpu.make_async_copy(
                    kv_buf.at[blk, j], kv_buf.at[blk, j], kv_recv.at[step, j]
                ).wait()

    def kv_forward(step):
        blk = jnp.maximum(e_pos - step, 0)

        @pl.when((e_pos - step >= 0) & (e_pos + 1 < n_ep))
        def _():
            for copy in kv_copy(step, kv_buf.at[blk, 0], kv_buf.at[blk, 1]):
                copy.start()

    mate = t_pos + 1 - 2 * (t_pos % 2)
    across = (t_pos + 2) % n_tp

    def shared_first(target, s, c):
        cols = pl.ds(c * wide, wide)
        return pltpu.make_async_remote_copy(
            src_ref=shared_ref.at[:, cols],
            dst_ref=sh_buf.at[t_pos, :, cols],
            send_sem=sh_send.at[s, c],
            recv_sem=sh_recv.at[s, c],
            device_id={"tp": target},
            device_id_type=MESH,
        )

    def shared_send(c):
        shared_first(mate, 0, c).start()
        shared_first(across, 1, c).start()

    @pl.when(e_pos + 1 < n_ep)
    def _():
        for copy in kv_copy(0, kn_ref, v_ref):
            copy.start()

    dispatch(0)
    dispatch(1)
    shared_send(0)
    acc_g[...] = jnp.zeros(acc_g.shape, F32)
    acc_u[...] = jnp.zeros(acc_u.shape, F32)
    owner = lax.broadcasted_iota(jnp.int32, acc_g.shape, 0) % local_count
    for c in range(CHUNKS):
        pltpu.make_async_copy(
            x_buf.at[c, pl.ds(0, peer_rows)], x_buf.at[c, pl.ds(0, peer_rows)], x_recv.at[c]
        ).wait()
        pltpu.make_async_copy(
            x_buf.at[c, pl.ds(0, group)], x_buf.at[c, pl.ds(0, group)], x_own.at[c]
        ).wait()
        if c < n_ep - 2:
            kv_arrived(c)
            kv_forward(c + 1)
        if c + 2 < CHUNKS:
            dispatch(c + 2)
            shared_send(c + 1)
        if c == CHUNKS - 2:
            shared_send(CHUNKS - 1)

        def one(e, carry):
            n = c * local_count + e
            slot = n % SLOTS
            for copy in weight_copies(n, slot):
                copy.wait()
            x = x_buf[c]
            mine = owner == e
            g = jnp.dot(x, ring[slot, 0], preferred_element_type=F32)
            acc_g[...] += jnp.where(mine, g, 0.0)
            u = jnp.dot(x, ring[slot, 1], preferred_element_type=F32)
            acc_u[...] += jnp.where(mine, u, 0.0)

            @pl.when(n + SLOTS < steps)
            def _():
                for copy in weight_copies(n + SLOTS, slot):
                    copy.start()

            return carry

        lax.fori_loop(0, local_count, one, 0)

    g = acc_g[...]
    hidden = (g / (1.0 + jnp.exp(-g))) * acc_u[...]
    width = acc_g.shape[1]
    for e in range(local_count):
        hid[:, e * width : (e + 1) * width] = jnp.where(owner == e, hidden, 0.0).astype(BF16)
    down_copy.wait()

    for c in range(CHUNKS):
        cols = pl.ds(c * wide, wide)
        half = wide // 2

        def tile(i, carry):
            y_buf[c, :, pl.ds(pl.multiple_of(i * half, half), half)] = jnp.dot(
                hid[...],
                down_buf[:, pl.ds(pl.multiple_of(c * wide + i * half, half), half)],
                preferred_element_type=F32,
            ).astype(BF16)
            return carry

        lax.fori_loop(0, 2, tile, 0)
        pltpu.make_async_copy(
            y_buf.at[c, rows_of(me)], r_buf.at[c, rows_of(me)], y_own.at[c]
        ).start()

        def give(i, carry):
            peer = (me + i) % count
            pltpu.make_async_remote_copy(
                src_ref=y_buf.at[c, rows_of(peer)],
                dst_ref=r_buf.at[c, rows_of(me)],
                send_sem=y_send.at[c],
                recv_sem=y_recv.at[c],
                device_id=device(peer),
                device_id_type=MESH,
            ).start()
            return carry

        lax.fori_loop(1, count, give, 0)

    for step in range(max(n_ep - 2, 0), n_ep - 1):
        kv_arrived(step)
    for copy in own_kv:
        copy.wait()

    across_copies = []
    for c in range(CHUNKS):
        cols = pl.ds(c * wide, wide)
        pltpu.make_async_copy(
            sh_buf.at[across, :, cols], sh_buf.at[across, :, cols], sh_recv.at[1, c]
        ).wait()
        copy = pltpu.make_async_remote_copy(
            src_ref=sh_buf.at[across, :, cols],
            dst_ref=sh_buf.at[across, :, cols],
            send_sem=sf_send.at[c],
            recv_sem=sf_recv.at[c],
            device_id={"tp": mate},
            device_id_type=MESH,
        )
        copy.start()
        across_copies.append(copy)

    size = qn_ref.shape[1] // heads
    rows = qn_ref.shape[0]
    length = n_ep * rows
    at = e_pos * rows + lax.broadcasted_iota(jnp.int32, (rows, length), 0)
    allowed = lax.broadcasted_iota(jnp.int32, (rows, length), 1) <= at
    contract = (((1,), (1,)), ((), ()))
    for h in range(heads):
        span = slice(h * size, (h + 1) * size)
        q = qn_ref[:, span]
        scores = jnp.concatenate(
            [
                lax.dot_general(q, kv_buf[blk, 0, :, span], contract, preferred_element_type=F32)
                for blk in range(n_ep)
            ],
            axis=1,
        )
        scores = scores * (size**-0.5) + qc_ref[:, h : h + 1] - kc_ref[h : h + 1, :]
        scores = jnp.where(allowed, scores, -1e30)
        top = jnp.max(scores, axis=1, keepdims=True)
        weights = jnp.where(allowed, jnp.exp(scores - top), 0.0)
        total = jnp.sum(weights, axis=1, keepdims=True)
        weights = weights.astype(BF16)
        mixed = jnp.zeros((rows, size), F32)
        for blk in range(n_ep):
            mixed += jnp.dot(
                weights[:, blk * rows : (blk + 1) * rows],
                kv_buf[blk, 1, :, span],
                preferred_element_type=F32,
            )
        att_ref[:, span] = (mixed / total).astype(BF16)

    own_shared.wait()
    third = mate + 2 - 4 * (mate // 2)
    for c in range(CHUNKS):
        cols = pl.ds(c * wide, wide)
        pltpu.make_async_copy(
            sh_buf.at[mate, :, cols], sh_buf.at[mate, :, cols], sh_recv.at[0, c]
        ).wait()
        pltpu.make_async_copy(
            sh_buf.at[third, :, cols], sh_buf.at[third, :, cols], sf_recv.at[c]
        ).wait()
    part = shared_ref.shape[0] // 3
    normed = normed_ref[...]
    hidden_parts = []
    for blk in range(n_tp):
        g = lax.dot_general(normed, sh_buf[blk, 0:part, :], contract, preferred_element_type=F32)
        u = lax.dot_general(
            normed, sh_buf[blk, part : 2 * part, :], contract, preferred_element_type=F32
        )
        hidden_parts.append(((g / (1.0 + jnp.exp(-g))) * u).astype(BF16))
    narrow = wide // 2
    for c in range(2 * CHUNKS):
        cols = slice(c * narrow, (c + 1) * narrow)
        total = jnp.zeros((normed.shape[0], narrow), F32)
        for blk in range(n_tp):
            piece = jnp.dot(
                hidden_parts[blk],
                sh_buf[blk, 2 * part : 3 * part, cols],
                preferred_element_type=F32,
            )
            total += piece.astype(BF16).astype(F32)
        sh_out[:, cols] = total.astype(BF16)

    for c in range(CHUNKS):
        pltpu.make_async_copy(
            r_buf.at[c, pl.ds(0, peer_rows)], r_buf.at[c, pl.ds(0, peer_rows)], y_recv.at[c]
        ).wait()
        pltpu.make_async_copy(
            r_buf.at[c, pl.ds(0, group)], r_buf.at[c, pl.ds(0, group)], y_own.at[c]
        ).wait()
        back = r_buf[c]
        routed = jnp.dot(high_ref[...], back, preferred_element_type=F32) + jnp.dot(
            low_ref[...], back, preferred_element_type=F32
        )
        cols = slice(c * wide, (c + 1) * wide)
        res_ref[:, cols] = (sh_out[:, cols].astype(F32) + routed).astype(BF16)

    for c in range(CHUNKS):
        pltpu.make_async_copy(
            x_buf.at[c, pl.ds(0, peer_rows)], x_buf.at[c, pl.ds(0, peer_rows)], x_send.at[c]
        ).wait()
        pltpu.make_async_copy(
            y_buf.at[c, pl.ds(0, peer_rows)], y_buf.at[c, pl.ds(0, peer_rows)], y_send.at[c]
        ).wait()
        shared_first(mate, 0, c).wait_send()
        shared_first(across, 1, c).wait_send()
        across_copies[c].wait_send()
    for step in range(n_ep - 1):

        @pl.when((e_pos - step >= 0) & (e_pos + 1 < n_ep))
        def _():
            for copy in kv_copy(step, kn_ref, v_ref):
                copy.wait_send()


def fused_local(n_ep, n_tp, *args):
    (
        queries,
        key_vectors,
        values,
        forget_cum,
        query_gain,
        key_gain,
        tokens,
        norm_gain,
        routes,
        route_weights,
        expert_gate,
        expert_up,
        expert_down,
        shared_gate,
        shared_up,
        shared_down,
    ) = args
    rows, heads, size = queries.shape
    row_count, dim = tokens.shape
    local_count, _, hidden = expert_gate.shape
    count = n_ep * n_tp
    slots = count * local_count * CAP
    part = shared_gate.shape[1]
    flat = heads * size
    vmem = pl.BlockSpec(memory_space=pltpu.VMEM)
    hbm = pl.BlockSpec(memory_space=pltpu.HBM)
    sds = jax.ShapeDtypeStruct
    normed, outgoing, high, low, query_norm, key_norm = pl.pallas_call(
        functools.partial(prepare_kernel, local_count, heads),
        out_shape=(
            sds((row_count, dim), BF16),
            sds((slots, dim), BF16),
            sds((row_count, slots), BF16),
            sds((row_count, slots), BF16),
            sds((rows, flat), BF16),
            sds((rows, flat), BF16),
        ),
        in_specs=[vmem] * 9,
        out_specs=[vmem] * 6,
        name="prepare",
    )(
        tokens,
        norm_gain.reshape(1, dim),
        routes,
        routes.T,
        route_weights,
        queries.reshape(rows, flat),
        key_vectors.reshape(rows, flat),
        query_gain.reshape(1, size),
        key_gain.reshape(1, size),
    )
    shared = jnp.concatenate([shared_gate.T, shared_up.T, shared_down], axis=0)
    query_cum = lax.dynamic_slice_in_dim(forget_cum, lax.axis_index("ep") * rows, rows, 0)
    wide = dim // CHUNKS
    dma = pltpu.SemaphoreType.DMA
    attended, routed = pl.pallas_call(
        functools.partial(fused_kernel, n_ep, n_tp, heads),
        out_shape=(sds((rows, flat), BF16), sds((row_count, dim), BF16)),
        in_specs=[vmem] * 6 + [hbm] * 7,
        out_specs=[vmem] * 2,
        scratch_shapes=[
            pltpu.VMEM((CHUNKS, slots, wide), BF16),
            pltpu.VMEM((CHUNKS, slots, wide), BF16),
            pltpu.VMEM((CHUNKS, slots, wide), BF16),
            pltpu.VMEM((SLOTS, 2, wide, hidden), BF16),
            pltpu.VMEM((local_count * hidden, dim), BF16),
            pltpu.VMEM((n_tp, 3 * part, dim), BF16),
            pltpu.VMEM((n_ep, 2, rows, flat), BF16),
            pltpu.VMEM((slots, hidden), F32),
            pltpu.VMEM((slots, hidden), F32),
            pltpu.VMEM((slots, local_count * hidden), BF16),
            pltpu.VMEM((row_count, dim), BF16),
            dma((CHUNKS,)),
            dma((CHUNKS,)),
            dma((CHUNKS,)),
            dma((CHUNKS,)),
            dma((CHUNKS,)),
            dma((CHUNKS,)),
            dma((SLOTS, 2)),
            dma,
            dma((2, CHUNKS)),
            dma((2, CHUNKS)),
            dma,
            dma((CHUNKS,)),
            dma((CHUNKS,)),
            dma((n_ep - 1, 2)),
            dma((n_ep - 1, 2)),
            dma((2,)),
        ],
        compiler_params=pltpu.CompilerParams(
            collective_id=0, has_side_effects=True, vmem_limit_bytes=60 * 1024 * 1024
        ),
        name="fused",
    )(
        normed,
        high,
        low,
        query_norm,
        query_cum,
        forget_cum.T,
        outgoing,
        key_norm,
        values.reshape(rows, flat),
        expert_gate,
        expert_up,
        expert_down.reshape(local_count * hidden, dim),
        shared,
    )
    return attended.reshape(rows, heads, size), routed


def local_of(mesh):
    n_ep, n_tp = mesh.shape["ep"], mesh.shape["tp"]

    def run(*args):
        experts = args[10]
        group = CAP * experts.shape[0]
        if n_tp == 4 and n_ep == 4 and group % 16 == 0 and args[15].shape[0] % 16 == 0:
            return fused_local(n_ep, n_tp, *args)
        return local(*args)

    return run


def solution(mesh):
    placed = (
        P(("grp", "ep"), "tp", None),
        P(("grp", "ep"), "tp", None),
        P(("grp", "ep"), "tp", None),
        P("grp", "tp"),
        P(),
        P(),
        P(("grp", "ep", "tp"), None),
        P(),
        P(("grp", "ep", "tp"), None),
        P(("grp", "ep", "tp"), None),
        P(("ep", "tp"), None, None),
        P(("ep", "tp"), None, None),
        P(("ep", "tp"), None, None),
        P(None, "tp"),
        P(None, "tp"),
        P("tp", None),
    )
    return jax.shard_map(
        local_of(mesh),
        mesh=mesh,
        in_specs=placed,
        out_specs=(P(("grp", "ep"), "tp", None), P(("grp", "ep", "tp"), None)),
        check_vma=False,
    )
```
